32 devices in a mesh: ep: 16 (over z, y, x), tp: 2 (over core).
Axes of the slice: x: 2, y: 2, z: 4, core: 2. Of those that a mesh axis runs over, the one named last changes fastest.
Arguments:
- tokens: bfloat16 [4096, 4096], P('ep'), may hold values from -6 to 6
- cotangent: bfloat16 [4096, 4096], P('ep'), may hold values from -1.5 to 1.5
- gates: float32 [4096, 2], P('ep'), may hold values from 0.05 to 0.95
- experts: int32 [4096, 2], P('ep'), may hold values from 0 to 15, all different within a row; in each aligned block of 256 rows (0 to 255, 256 to 511, ...) at most 48 rows name the same one
- gate_w: bfloat16 [16, 4096, 768], P('ep', None, 'tp'), may hold values from -0.09375 to 0.09375
- up_w: bfloat16 [16, 4096, 768], P('ep', None, 'tp'), may hold values from -0.09375 to 0.09375
- down_w: bfloat16 [16, 768, 4096], P('ep', 'tp'), may hold values from -0.21875 to 0.21875
Outputs:
- grad_tokens: bfloat16 [4096, 4096], P('ep', 'tp')
- grad_gates: float32 [4096, 2], P('ep')
- grad_gate_w: bfloat16 [16, 4096, 768], P('ep', None, 'tp')
- grad_up_w: bfloat16 [16, 4096, 768], P('ep', None, 'tp')
- grad_down_w: bfloat16 [16, 768, 4096], P('ep', 'tp')
- sq_gate: float32 [16, 4096], P('ep')
- sq_up: float32 [16, 4096], P('ep')
- sq_down: float32 [16, 768], P('ep', 'tp')
The draws below stay inside these ranges and needn't reach their ends.
Inputs may be any that keep to these rules, and one draw needn't show every extreme that they name: In each aligned block of 256 rows no expert is named by more than 48 rows, a bound that some expert reaches in some blocks; the 2 experts of a row differ.
All inputs are finite; a program needn't handle non-finite values.
Results may differ from the reference program's by a relative error of at most 0.024.
Values may be sent and summed in bfloat16 or wider, within the bound.
A program may use at most 192 MiB of HBM per device.

```python
import math
import jax
import jax.numpy as jnp
import numpy as np
from jax import lax

D = 4096
FF = 768
TOPK = 2
TOK_DEV = 256
EXPERTS = 16
CAP = 48
TOKENS = 4096
N_EP = 16
N_TP = 2


def level_of(key, dims, shards, low, top_value):
    factor_of, own = 1.0, jax.random.fold_in(key, 6)
    for position, shards_of in shards:
        heights = jnp.exp(jax.random.uniform(jax.random.fold_in(own, position), (shards_of,), jnp.float32, low / len(shards), top_value / len(shards)))
        factor_of = factor_of * jnp.repeat(heights, dims[position] // shards_of).reshape([-1 if axis == position else 1 for axis in range(len(dims))])
    return factor_of


def shared_out(own_key, own, number, rows, number_of, top, bound, lean):
    sequence = jax.random.permutation(own_key, number_of)
    crowded, ordinary = load_shares(number_of, rows * top, bound, lean, True), load_shares(number_of, rows * top, bound, lean, False)
    places = jnp.arange(number_of)

    def named(sizes, offset_by):
        used = int((sizes > 0).sum())
        fixed = max(1, used // 4)
        moved = fixed + (places - fixed + offset_by * (used - fixed)) % max(1, number_of - fixed)
        return jnp.zeros((number_of,), jnp.int32).at[sequence[jnp.where(places < fixed, places, moved)]].set(jnp.asarray(sizes, jnp.int32))

    sizes = jnp.where(number % 4 == 0, named(crowded, number // 4), named(ordinary, number - number // 4 - 1))
    mixed = jax.random.permutation(jax.random.fold_in(own, 3), number_of)
    source_of, sink = mixed[0:number_of // 2 * 2:2], mixed[1:number_of // 2 * 2:2]
    slack = jnp.minimum(sizes[source_of] - 1, bound - sizes[sink]) // 2
    slack = jnp.where((source_of == sequence[0]) | (sink == sequence[0]) | (sizes[sink] == 0), 0, jnp.maximum(slack, 0))
    moved = jax.random.randint(jax.random.fold_in(own, 4), (number_of // 2,), 0, 1 << 20) % (slack + 1)
    sizes = sizes.at[source_of].add(-moved).at[sink].add(moved)
    items = jnp.searchsorted(jnp.cumsum(sizes), jnp.arange(rows * top), side="right").astype(jnp.int32)
    grid = items.reshape(top, rows).T
    grid = grid[jax.random.permutation(jax.random.fold_in(own, 1), rows)]
    offset_by = jax.random.randint(jax.random.fold_in(own, 2), (rows, 1), 0, top)
    return jnp.take_along_axis(grid, (jnp.arange(top)[None, :] + offset_by) % top, axis=1)


def load_shares(number_of, total, limit, lean, full):
    weights = [(1 << 20) // math.isqrt(grade ** lean) + 1 for grade in range(1, number_of + 1)]
    largest = limit if full else min(limit, max(-(-total // number_of), total * weights[0] // sum(weights)))
    least = 1 if total - largest >= number_of - 1 else 0
    given, rest = [largest] + [least] * (number_of - 1), total - largest - least * (number_of - 1)
    while rest > 0:
        movable = [i for i in range(1, number_of) if given[i] < largest] or [i for i in range(1, number_of) if given[i] < limit]
        whole, budget = sum([weights[i] for i in movable]), rest
        for i in movable:
            addition = min(limit - given[i], max(1, budget * weights[i] // whole), rest)
            given[i] = given[i] + addition
            rest = rest - addition
    return np.array(given)


def bell_draw(key, extent, width, most, split=(), kind=jnp.bfloat16):
    array = jax.random.normal(key, extent, jnp.float32) * width
    if len(split) > 0:
        array = level_of(key, extent, split, -0.22, 0.18) * array
    return jnp.clip(array, min=-most, max=most).astype(kind)


def setup_inputs(seed: int = 0) -> dict:
    streams_of = jax.random.split(jax.random.key(seed), 8)
    tokens = bell_draw(streams_of[0], (TOKENS, D), 1.0, 6.0, ((0, 16),))
    cotangent = bell_draw(streams_of[1], (TOKENS, D), 0.25, 1.5, ((0, 16),))
    gates = jnp.clip(0.05 + 0.9 * jax.random.uniform(streams_of[2], (TOKENS, TOPK), jnp.float32) ** level_of(streams_of[2], (TOKENS, TOPK), ((0, 16),), -0.2, 0.2), 0.05, 0.95)
    experts_keys = jax.random.split(jax.random.fold_in(streams_of[3], 1), TOKENS // TOK_DEV)
    experts_turns = jax.random.permutation(jax.random.fold_in(streams_of[3], 3), TOKENS // TOK_DEV)
    experts = jax.vmap(lambda own, number: shared_out(jax.random.fold_in(streams_of[3], 2), own, number, TOK_DEV, EXPERTS, TOPK, CAP, 2))(experts_keys, experts_turns).reshape((TOKENS, TOPK))
    gate_w = bell_draw(streams_of[4], (EXPERTS, D, FF), D ** -0.5, 0.09375, ((0, 16), (2, 2)))
    up_w = bell_draw(streams_of[5], (EXPERTS, D, FF), D ** -0.5, 0.09375, ((0, 16), (2, 2)))
    down_w = bell_draw(streams_of[6], (EXPERTS, FF, D), FF ** -0.5, 0.21875, ((0, 16), (1, 2)))
    return dict(tokens=tokens, cotangent=cotangent, gates=gates, experts=experts, gate_w=gate_w, up_w=up_w, down_w=down_w)


def expert_terms(w_gate, w_up, w_down, indices, tokens, cotangent, gates):
    n_assign = TOKENS * TOPK
    valid = indices < n_assign
    safe = jnp.minimum(indices, n_assign - 1)
    tok_index = safe // TOPK
    rows_x = jnp.where(valid[:, None], tokens[tok_index], jnp.zeros((), jnp.bfloat16)).astype(jnp.bfloat16)
    rows_dy = jnp.where(valid[:, None], cotangent[tok_index], jnp.zeros((), jnp.bfloat16)).astype(jnp.bfloat16)
    rows_g = jnp.where(valid, gates.reshape(-1)[safe], jnp.zeros((), jnp.float32))
    pre_gate = jnp.dot(rows_x, w_gate, preferred_element_type=jnp.float32)
    pre_up = jnp.dot(rows_x, w_up, preferred_element_type=jnp.float32)
    sigmoid_gate = jax.nn.sigmoid(pre_gate)
    silu_gate = pre_gate * sigmoid_gate
    hidden = (silu_gate * pre_up).astype(jnp.bfloat16)
    hidden_grad = jnp.dot(rows_dy, w_down.T, preferred_element_type=jnp.float32)
    gate_sum = jnp.sum(hidden.astype(jnp.float32) * hidden_grad, axis=1)
    scaled = rows_g[:, None] * hidden_grad
    grad_pre_gate = (scaled * pre_up * sigmoid_gate * (1.0 + pre_gate * (1.0 - sigmoid_gate))).astype(jnp.bfloat16)
    grad_pre_up = (scaled * silu_gate).astype(jnp.bfloat16)
    weighted = (rows_g[:, None] * hidden.astype(jnp.float32)).astype(jnp.bfloat16)
    grad_dw = jnp.dot(weighted.T, rows_dy, preferred_element_type=jnp.float32).astype(jnp.bfloat16)
    grad_gw = jnp.dot(rows_x.T, grad_pre_gate, preferred_element_type=jnp.float32).astype(jnp.bfloat16)
    grad_uw = jnp.dot(rows_x.T, grad_pre_up, preferred_element_type=jnp.float32).astype(jnp.bfloat16)
    rows = rows_x.shape[0]
    block_units = FF // N_TP
    split_gate = grad_pre_gate.astype(jnp.float32).reshape(rows, N_TP, block_units)
    split_up = grad_pre_up.astype(jnp.float32).reshape(rows, N_TP, block_units)
    wg_split = w_gate.astype(jnp.float32).reshape(D, N_TP, block_units)
    wu_split = w_up.astype(jnp.float32).reshape(D, N_TP, block_units)
    partial_value = jnp.einsum('rhf,dhf->rhd', split_gate, wg_split) + jnp.einsum('rhf,dhf->rhd', split_up, wu_split)
    partial_value = partial_value.astype(jnp.bfloat16).astype(jnp.float32)
    row_grad = jnp.sum(partial_value, axis=1).astype(jnp.bfloat16)
    return grad_gw, grad_uw, grad_dw, row_grad, gate_sum


def reference(tokens, cotangent, gates, experts, gate_w, up_w, down_w):
    n_assign = TOKENS * TOPK
    flat_ids = experts.reshape(N_EP, TOK_DEV * TOPK)
    onehot = (flat_ids[:, :, None] == jnp.arange(EXPERTS, dtype=jnp.int32)[None, None, :]).astype(jnp.int32)
    earlier = jnp.cumsum(onehot, axis=1) - onehot
    slot_of = jnp.sum(earlier * onehot, axis=2).astype(jnp.int32)
    block_id = jnp.broadcast_to(jnp.arange(N_EP, dtype=jnp.int32)[:, None], flat_ids.shape)
    numbers = jnp.arange(n_assign, dtype=jnp.int32).reshape(N_EP, TOK_DEV * TOPK)
    table = jnp.full((EXPERTS, N_EP, CAP), n_assign, jnp.int32).at[flat_ids, block_id, slot_of].set(numbers)
    table = table.reshape(EXPERTS, N_EP * CAP)

    def per_expert(args):
        w_gate, w_up, w_down, indices = args
        return expert_terms(w_gate, w_up, w_down, indices, tokens, cotangent, gates)

    grad_gw, grad_uw, grad_dw, row_grad, gate_sum = lax.map(per_expert, (gate_w, up_w, down_w, table))
    flat_index = table.reshape(-1)
    tok_target = jnp.where(flat_index < n_assign, flat_index // TOPK, TOKENS).astype(jnp.int32)
    grad_tokens = jnp.zeros((TOKENS, D), jnp.float32).at[tok_target].add(
        row_grad.reshape(-1, D).astype(jnp.float32), mode="drop").astype(jnp.bfloat16)
    grad_gates = jnp.zeros((n_assign,), jnp.float32).at[flat_index].set(
        gate_sum.reshape(-1), mode="drop").reshape(TOKENS, TOPK)
    gw_f = grad_gw.astype(jnp.float32)
    uw_f = grad_uw.astype(jnp.float32)
    dw_f = grad_dw.astype(jnp.float32)
    sq_gate = jnp.sum(gw_f * gw_f, axis=2) / FF
    sq_up = jnp.sum(uw_f * uw_f, axis=2) / FF
    sq_down = jnp.sum(dw_f * dw_f, axis=2) / D
    return (grad_tokens, grad_gates, grad_gw, grad_uw, grad_dw, sq_gate, sq_up, sq_down)
```

```python
import functools

import jax
import jax.numpy as jnp
from jax import lax
from jax.experimental import pallas as pl
from jax.experimental.pallas import tpu as pltpu
from jax.sharding import PartitionSpec as P

MESH = pl.DeviceIdType.MESH
BF16 = jnp.bfloat16
F32 = jnp.float32
NN = (((1,), (0,)), ((), ()))
NT = (((1,), (1,)), ((), ()))
TN = (((0,), (0,)), ((), ()))


def dot(a, b, dims, precision=None):
    return lax.dot_general(a, b, dims, precision=precision, preferred_element_type=F32)


def kernel(
    n, cap, units, share, groups, tile,
    sx, sdy, sg, wg_in, wu_in, wd_in,
    back, gback, ggw, guw, gdw, sq_out, sqd_out,
    xr, dyr, gr, wg, wu, wd, pg, pu, prod, gpgu, wt, keep, give, got, rg,
    gp, gpp, gt, gcol, sqs, sqr, acc,
    w_sem, s_sem, r_sem, gs_sem, gr_sem, fs_sem, fr_sem,
    ps_sem, pr_sem, qs_sem, qr_sem, bs_sem, br_sem, hs_sem, hr_sem, o_sem, e_sem,
):
    me = lax.axis_index("ep")
    t = lax.axis_index("tp")
    other = lax.axis_size("tp") - 1 - t
    per = n // groups
    rows_g = per * cap

    def rows(s):
        return pl.ds(pl.multiple_of(s * cap, 16), cap)

    def remote(src, dst, send, recv, **where):
        return pltpu.make_async_remote_copy(
            src_ref=src, dst_ref=dst, send_sem=send, recv_sem=recv,
            device_id=where, device_id_type=MESH,
        )

    def loop(count, fn):
        def step(i, carry):
            fn(i)
            return carry
        lax.fori_loop(0, count, step, 0)

    def peer(k):
        return lax.rem(me + n // 2 + k + jnp.where(k >= n - n // 2, 1, 0), n)

    barrier = pltpu.get_barrier_semaphore()
    loop(n - 1, lambda k: pl.semaphore_signal(
        barrier, inc=1, device_id={"ep": peer(k)}, device_id_type=MESH))
    pl.semaphore_signal(barrier, inc=1, device_id={"tp": other}, device_id_type=MESH)
    pl.semaphore_wait(barrier, n)

    ins = ((sx, xr), (sdy, dyr))
    for which, (src, dst) in enumerate(ins):
        def send(k, which=which, src=src, dst=dst):
            d = peer(k)
            remote(src.at[d], dst.at[t, rows(me)], s_sem.at[which, d],
                   r_sem.at[which, me], ep=d).start()
        loop(n - 1, send)
        pltpu.make_async_copy(src.at[me], dst.at[t, rows(me)], r_sem.at[which, me]).start()
        if which == 0:
            def send_gate(k):
                d = peer(k)
                remote(sg.at[d], gr.at[me], gs_sem.at[d], gr_sem.at[me], ep=d).start()
            loop(n - 1, send_gate)
            pltpu.make_async_copy(sg.at[me], gr.at[me], gr_sem.at[me]).start()
            loads = [
                pltpu.make_async_copy(a, b, w_sem.at[i])
                for i, (a, b) in enumerate(((wg_in, wg), (wu_in, wu), (wd_in, wd)))
            ]
            for load in loads:
                load.start()

    def order(i):
        return lax.rem(me // per + groups // 2 + i, groups)

    def arrive(which, g):
        src, dst = ins[which]

        def pass_on(j):
            s = g * per + j
            pltpu.make_async_copy(src.at[0], dst.at[t, rows(s)], r_sem.at[which, s]).wait()
            remote(dst.at[t, rows(s)], dst.at[t, rows(s)], fs_sem.at[which, s],
                   fr_sem.at[which, s], tp=other).start()

        def joined(j):
            s = g * per + j
            remote(dst.at[other, rows(s)], dst.at[other, rows(s)], fs_sem.at[which, s],
                   fr_sem.at[which, s], tp=other).wait_recv()

        loop(per, pass_on)
        loop(per, joined)

    def span(g):
        return pl.ds(pl.multiple_of(g * rows_g, 16), rows_g)

    for load in loads:
        load.wait()

    def forward(i):
        g = order(i)
        arrive(0, g)
        r = span(g)
        pg[r, :] = dot(xr[0, r, :], wg[0], NN) + dot(xr[1, r, :], wg[1], NN)
        pu[r, :] = dot(xr[0, r, :], wu[0], NN) + dot(xr[1, r, :], wu[1], NN)

    loop(groups, forward)

    def exchange(g):
        r = span(g)
        grp = pl.ds(g * per, per)
        return (
            remote(give.at[r], got.at[r], ps_sem.at[g], pr_sem.at[g], tp=other),
            remote(gp.at[grp], gpp.at[grp], qs_sem.at[g], qr_sem.at[g], tp=other),
        )

    def back_copies(s):
        return (
            remote(rg.at[rows(s)], back.at[me], bs_sem.at[s], br_sem.at[me], ep=s),
            remote(gt.at[s], gback.at[me], hs_sem.at[s], hr_sem.at[me], ep=s),
        )

    def finish(g):
        for copy in exchange(g):
            copy.wait_recv()

        def one(j):
            s = g * per + j
            r = rows(s)
            rg[r, :] = (keep[r, :].astype(F32) + got[r, :].astype(F32)).astype(BF16)
            gt[s] = gp[s] + gpp[s]

        loop(per, one)

        def out(j):
            s = g * per + j

            @pl.when(s == me)
            def _():
                pltpu.make_async_copy(rg.at[rows(s)], back.at[me], br_sem.at[me]).start()
                pltpu.make_async_copy(gt.at[s], gback.at[me], hr_sem.at[me]).start()

            @pl.when(s != me)
            def _():
                for copy in back_copies(s):
                    copy.start()

        loop(per, out)

    ones_units = jnp.ones((8, units), F32)

    def backward(i):
        g = order(i)
        arrive(1, g)

        def gates_in(j):
            s = g * per + j
            pltpu.make_async_copy(sg.at[0], gr.at[s], gr_sem.at[s]).wait()
            column = jnp.transpose(gr[s])
            gcol[rows(s), :] = jnp.broadcast_to(column[:cap, 0:1], (cap, 128))

        loop(per, gates_in)
        r = span(g)
        dh = dot(dyr[0, r, :], wd[:, :share], NT) + dot(dyr[1, r, :], wd[:, share:], NT)
        a = pg[r, :]
        b = pu[r, :]
        gate = gcol[r, 0:1]
        sig = jax.nn.sigmoid(a)
        silu = a * sig
        hidden = (silu * b).astype(BF16).astype(F32)
        prod[...] = hidden * dh
        scaled = gate * dh
        gpg = (scaled * b * sig * (1.0 + a * (1.0 - sig))).astype(BF16)
        gpu = (scaled * silu).astype(BF16)
        gpgu[r, :units] = gpg
        gpgu[r, units:] = gpu
        wt[r, :] = (gate * hidden).astype(BF16)

        def part(c):
            cols = pl.ds(pl.multiple_of(c * tile, tile), tile)
            for half, dst in ((other, give), (t, keep)):
                dst[r, cols] = (
                    dot(gpgu[r, :units], wg[half, cols, :], NT)
                    + dot(gpgu[r, units:], wu[half, cols, :], NT)
                ).astype(BF16)

        loop(share // tile, part)

        def gate_sum(j):
            p = prod[pl.ds(pl.multiple_of(j * cap, 16), cap), :]
            gp[g * per + j, :, :cap] = dot(ones_units, p, NT, lax.Precision.HIGHEST)

        loop(per, gate_sum)
        for copy in exchange(g):
            copy.start()

        @pl.when(i > 0)
        def _():
            finish(order(i - 1 + groups))

    gp[...] = jnp.zeros_like(gp)
    loop(groups, backward)
    finish(order(groups - 1))

    acc[...] = jnp.zeros_like(acc)
    for h in range(2):
        def grads(c, h=h):
            cols = pl.ds(pl.multiple_of(c * tile, tile), tile)
            q = dot(xr[h, :, cols], gpgu[...], TN).astype(BF16)
            wg[h, cols, :] = q[:, :units]
            wu[h, cols, :] = q[:, units:]
            f = q.astype(F32)
            f = f * f
            sqs[0, h, c] = dot(ones_units, f[:, :units], NT, lax.Precision.HIGHEST)
            sqs[1, h, c] = dot(ones_units, f[:, units:], NT, lax.Precision.HIGHEST)
            d = dot(wt[...], dyr[h, :, cols], TN).astype(BF16)
            wd[:, pl.ds(pl.multiple_of(h * share + c * tile, tile), tile)] = d
            d = d.astype(F32)
            acc[...] += d * d

        loop(share // tile, grads)

    stores = [
        pltpu.make_async_copy(a, b, o_sem.at[i])
        for i, (a, b) in enumerate(((wg, ggw), (wu, guw), (wd, gdw)))
    ]
    for store in stores:
        store.start()
    squares = remote(sqs, sqr, e_sem.at[0], e_sem.at[1], tp=other)
    squares.start()
    sqd_out[...] = dot(jnp.ones((8, tile), F32), acc[...], NT, lax.Precision.HIGHEST)
    squares.wait()
    sq_out[...] = sqs[...] + sqr[...]
    for store in stores:
        store.wait()

    def drain(k):
        d = peer(k)
        for which, (src, dst) in enumerate(ins):
            remote(src.at[d], dst.at[t, rows(me)], s_sem.at[which, d],
                   r_sem.at[which, me], ep=d).wait_send()
        remote(sg.at[d], gr.at[me], gs_sem.at[d], gr_sem.at[me], ep=d).wait_send()
        for copy in back_copies(d):
            copy.wait_send()

    loop(n - 1, drain)

    def drain_pair(s):
        for which, (src, dst) in enumerate(ins):
            remote(dst.at[t, rows(s)], dst.at[t, rows(s)], fs_sem.at[which, s],
                   fr_sem.at[which, s], tp=other).wait_send()
        pltpu.make_async_copy(rg.at[rows(s)], back.at[s], br_sem.at[s]).wait()
        pltpu.make_async_copy(gt.at[s], gback.at[s], hr_sem.at[s]).wait()

    loop(n, drain_pair)

    def drain_group(g):
        for copy in exchange(g):
            copy.wait_send()

    loop(groups, drain_group)


def fused(n, cap, send_x, send_dy, send_gate, w_gate, w_up, w_down):
    width, units = w_gate.shape
    share = send_x.shape[2]
    total = n * cap
    groups = 4
    tile = 512
    any_spec = pl.BlockSpec(memory_space=pl.ANY)
    vmem = pl.BlockSpec(memory_space=pltpu.VMEM)
    sq_shape = (2, 2, share // tile, 8, tile)
    dma = pltpu.SemaphoreType.DMA
    shape = jax.ShapeDtypeStruct
    return pl.pallas_call(
        functools.partial(kernel, n, cap, units, share, groups, tile),
        out_shape=(
            shape((n, cap, share), BF16),
            shape((n, 8, 128), F32),
            shape((2, share, units), BF16),
            shape((2, share, units), BF16),
            shape((units, width), BF16),
            shape(sq_shape, F32),
            shape((8, units), F32),
        ),
        in_specs=[any_spec] * 6,
        out_specs=(any_spec,) * 5 + (vmem, vmem),
        scratch_shapes=[
            pltpu.VMEM((2, total, share), BF16),
            pltpu.VMEM((2, total, share), BF16),
            pltpu.VMEM((n, 8, 128), F32),
            pltpu.VMEM((2, share, units), BF16),
            pltpu.VMEM((2, share, units), BF16),
            pltpu.VMEM((units, width), BF16),
            pltpu.VMEM((total, units), F32),
            pltpu.VMEM((total, units), F32),
            pltpu.VMEM((total // groups, units), F32),
            pltpu.VMEM((total, 2 * units), BF16),
            pltpu.VMEM((total, units), BF16),
            pltpu.VMEM((total, share), BF16),
            pltpu.VMEM((total, share), BF16),
            pltpu.VMEM((total, share), BF16),
            pltpu.VMEM((total, share), BF16),
            pltpu.VMEM((n, 8, 128), F32),
            pltpu.VMEM((n, 8, 128), F32),
            pltpu.VMEM((n, 8, 128), F32),
            pltpu.VMEM((total, 128), F32),
            pltpu.VMEM(sq_shape, F32),
            pltpu.VMEM(sq_shape, F32),
            pltpu.VMEM((units, tile), F32),
            dma((3,)), dma((2, n)), dma((2, n)), dma((n,)), dma((n,)), dma((2, n)), dma((2, n)),
            dma((groups,)), dma((groups,)), dma((groups,)), dma((groups,)),
            dma((n,)), dma((n,)), dma((n,)), dma((n,)), dma((3,)), dma((2,)),
        ],
        compiler_params=pltpu.CompilerParams(
            collective_id=0, has_side_effects=True, vmem_limit_bytes=63 << 20
        ),
    )(send_x, send_dy, send_gate,
      w_gate.reshape(2, share, units), w_up.reshape(2, share, units), w_down)


def body(tokens, cotangent, gates, experts, gate_w, up_w, down_w):
    tok_rows, width = tokens.shape
    top_count = experts.shape[1]
    n_ep = lax.axis_size("ep")
    n_cores = lax.axis_size("tp")
    capacity = 3 * tok_rows * top_count // (2 * n_ep)
    cap = -(-capacity // 16) * 16
    n_slots = n_ep * cap
    flat_ids = experts.reshape(-1)
    onehot = (flat_ids[:, None] == jnp.arange(n_ep, dtype=jnp.int32)[None, :]).astype(jnp.int32)
    earlier = jnp.cumsum(onehot, axis=0) - onehot
    slot_of = jnp.sum(earlier * onehot, axis=1)
    target = flat_ids * cap + slot_of
    placing = (target[None, :] == jnp.arange(n_slots, dtype=jnp.int32)[:, None]).astype(F32)
    place_tok = jnp.sum(placing.reshape(n_slots, tok_rows, top_count), axis=2).astype(BF16)
    send_gate = jnp.dot(placing, gates.reshape(-1), precision=lax.Precision.HIGHEST)
    send_gate = jnp.pad(send_gate.reshape(n_ep, 1, cap), ((0, 0), (0, 7), (0, 128 - cap)))
    share = width // n_cores
    offset = lax.axis_index("tp") * share
    tok_share = lax.dynamic_slice_in_dim(tokens, offset, share, 1)
    cot_share = lax.dynamic_slice_in_dim(cotangent, offset, share, 1)
    send_x = jnp.dot(place_tok, tok_share, preferred_element_type=F32).astype(BF16)
    send_dy = jnp.dot(place_tok, cot_share, preferred_element_type=F32).astype(BF16)
    back, gback, ggw, guw, gdw, sq, sqd = fused(
        n_ep, cap, send_x.reshape(n_ep, cap, share), send_dy.reshape(n_ep, cap, share),
        send_gate, gate_w[0], up_w[0], down_w[0],
    )
    grad_tokens = lax.dot_general(
        place_tok, back.reshape(n_slots, share), TN, preferred_element_type=F32
    ).astype(BF16)
    grad_gates = jnp.dot(
        gback[:, 0, :cap].reshape(n_slots), placing, precision=lax.Precision.HIGHEST
    ).reshape(tok_rows, top_count)
    full_units = gate_w.shape[2] * n_cores
    sq = sq[:, :, :, 0, :].reshape(2, width) / full_units
    return (
        grad_tokens,
        grad_gates,
        ggw.reshape(gate_w.shape),
        guw.reshape(up_w.shape),
        gdw[None],
        sq[0][None],
        sq[1][None],
        sqd[0:1] / width,
    )


def solution(mesh):
    placed = (
        P("ep", None),
        P("ep", None),
        P("ep", None),
        P("ep", None),
        P("ep", None, "tp"),
        P("ep", None, "tp"),
        P("ep", "tp", None),
    )
    return jax.shard_map(
        body,
        mesh=mesh,
        in_specs=placed,
        out_specs=(
            P("ep", "tp"),
            P("ep", None),
            P("ep", None, "tp"),
            P("ep", None, "tp"),
            P("ep", "tp", None),
            P("ep", None),
            P("ep", None),
            P("ep", "tp"),
        ),
        check_vma=False,
    )
```

```python
import functools

import jax
import jax.numpy as jnp
from jax import lax
from jax.experimental import pallas as pl
from jax.experimental.pallas import tpu as pltpu
from jax.sharding import PartitionSpec as P

MESH = pl.DeviceIdType.MESH
BF16 = jnp.bfloat16
F32 = jnp.float32
NN = (((1,), (0,)), ((), ()))
NT = (((1,), (1,)), ((), ()))
TN = (((0,), (0,)), ((), ()))


def dot(a, b, dims, precision=None):
    return lax.dot_general(a, b, dims, precision=precision, preferred_element_type=F32)


def kernel(
    n, cap, units, share, groups, tile,
    sx, sdy, sg, wg_in, wu_in, wd_in,
    back, gback, ggw, guw, gdw, sq_out, sqd_out,
    xr, dyr, gr, wg, wu, wd, pg, pu, prod, gpgu, wt, keep, give, got, rg,
    gp, gpp, gt, gcol, sqs, sqr, acc,
    w_sem, s_sem, r_sem, gs_sem, gr_sem, fs_sem, fr_sem,
    ps_sem, pr_sem, qs_sem, qr_sem, bs_sem, br_sem, hs_sem, hr_sem, o_sem, e_sem,
):
    me = lax.axis_index("ep")
    t = lax.axis_index("tp")
    other = lax.axis_size("tp") - 1 - t
    per = n // groups
    rows_g = per * cap

    def rows(s):
        return pl.ds(pl.multiple_of(s * cap, 16), cap)

    def remote(src, dst, send, recv, **where):
        return pltpu.make_async_remote_copy(
            src_ref=src, dst_ref=dst, send_sem=send, recv_sem=recv,
            device_id=where, device_id_type=MESH,
        )

    def loop(count, fn):
        def step(i, carry):
            fn(i)
            return carry
        lax.fori_loop(0, count, step, 0)

    def peer(k):
        return lax.rem(me + n // 2 + k + jnp.where(k >= n - n // 2, 1, 0), n)

    barrier = pltpu.get_barrier_semaphore()
    loop(n - 1, lambda k: pl.semaphore_signal(
        barrier, inc=1, device_id={"ep": peer(k)}, device_id_type=MESH))
    pl.semaphore_signal(barrier, inc=1, device_id={"tp": other}, device_id_type=MESH)
    pl.semaphore_wait(barrier, n)

    ins = ((sx, xr), (sdy, dyr))
    for which, (src, dst) in enumerate(ins):
        def send(k, which=which, src=src, dst=dst):
            d = peer(k)
            remote(src.at[d], dst.at[t, rows(me)], s_sem.at[which, d],
                   r_sem.at[which, me], ep=d).start()
        loop(n - 1, send)
        pltpu.make_async_copy(src.at[me], dst.at[t, rows(me)], r_sem.at[which, me]).start()
        if which == 0:
            def send_gate(k):
                d = peer(k)
                remote(sg.at[d], gr.at[me], gs_sem.at[d], gr_sem.at[me], ep=d).start()
            loop(n - 1, send_gate)
            pltpu.make_async_copy(sg.at[me], gr.at[me], gr_sem.at[me]).start()
            loads = [
                pltpu.make_async_copy(a, b, w_sem.at[i])
                for i, (a, b) in enumerate(((wg_in, wg), (wu_in, wu), (wd_in, wd)))
            ]
            for load in loads:
                load.start()

    def order(i):
        return lax.rem(me // per + groups // 2 + i, groups)

    def arrive(which, g):
        src, dst = ins[which]

        def pass_on(j):
            s = g * per + j
            pltpu.make_async_copy(src.at[0], dst.at[t, rows(s)], r_sem.at[which, s]).wait()
            remote(dst.at[t, rows(s)], dst.at[t, rows(s)], fs_sem.at[which, s],
                   fr_sem.at[which, s], tp=other).start()

        def joined(j):
            s = g * per + j
            remote(dst.at[other, rows(s)], dst.at[other, rows(s)], fs_sem.at[which, s],
                   fr_sem.at[which, s], tp=other).wait_recv()

        loop(per, pass_on)
        loop(per, joined)

    def span(g):
        return pl.ds(pl.multiple_of(g * rows_g, 16), rows_g)

    for load in loads:
        load.wait()

    def forward(i):
        g = order(i)
        arrive(0, g)
        r = span(g)
        pg[r, :] = dot(xr[0, r, :], wg[0], NN) + dot(xr[1, r, :], wg[1], NN)
        pu[r, :] = dot(xr[0, r, :], wu[0], NN) + dot(xr[1, r, :], wu[1], NN)

    loop(groups, forward)

    def exchange(g):
        r = span(g)
        grp = pl.ds(g * per, per)
        return (
            remote(give.at[r], got.at[r], ps_sem.at[g], pr_sem.at[g], tp=other),
            remote(gp.at[grp], gpp.at[grp], qs_sem.at[g], qr_sem.at[g], tp=other),
        )

    def back_copies(s):
        return (
            remote(rg.at[rows(s)], back.at[me], bs_sem.at[s], br_sem.at[me], ep=s),
            remote(gt.at[s], gback.at[me], hs_sem.at[s], hr_sem.at[me], ep=s),
        )

    def finish(g):
        for copy in exchange(g):
            copy.wait_recv()

        def one(j):
            s = g * per + j
            r = rows(s)
            rg[r, :] = (keep[r, :].astype(F32) + got[r, :].astype(F32)).astype(BF16)
            gt[s] = gp[s] + gpp[s]

        loop(per, one)

        def out(j):
            s = g * per + j

            @pl.when(s == me)
            def _():
                pltpu.make_async_copy(rg.at[rows(s)], back.at[me], br_sem.at[me]).start()
                pltpu.make_async_copy(gt.at[s], gback.at[me], hr_sem.at[me]).start()

            @pl.when(s != me)
            def _():
                for copy in back_copies(s):
                    copy.start()

        loop(per, out)

    ones_units = jnp.ones((8, units), F32)

    def backward(i):
        g = order(i)
        arrive(1, g)

        def gates_in(j):
            s = g * per + j
            pltpu.make_async_copy(sg.at[0], gr.at[s], gr_sem.at[s]).wait()
            column = jnp.transpose(gr[s])
            gcol[rows(s), :] = jnp.broadcast_to(column[:cap, 0:1], (cap, 128))

        loop(per, gates_in)
        r = span(g)
        dh = dot(dyr[0, r, :], wd[:, :share], NT) + dot(dyr[1, r, :], wd[:, share:], NT)
        a = pg[r, :]
        b = pu[r, :]
        gate = gcol[r, 0:1]
        sig = jax.nn.sigmoid(a)
        silu = a * sig
        hidden = (silu * b).astype(BF16).astype(F32)
        prod[...] = hidden * dh
        scaled = gate * dh
        gpg = (scaled * b * sig * (1.0 + a * (1.0 - sig))).astype(BF16)
        gpu = (scaled * silu).astype(BF16)
        gpgu[r, :units] = gpg
        gpgu[r, units:] = gpu
        wt[r, :] = (gate * hidden).astype(BF16)

        def part(c):
            cols = pl.ds(pl.multiple_of(c * tile, tile), tile)
            for half, dst in ((other, give), (t, keep)):
                dst[r, cols] = (
                    dot(gpgu[r, :units], wg[half, cols, :], NT)
                    + dot(gpgu[r, units:], wu[half, cols, :], NT)
                ).astype(BF16)

        loop(share // tile, part)

        def gate_sum(j):
            p = prod[pl.ds(pl.multiple_of(j * cap, 16), cap), :]
            gp[g * per + j, :, :cap] = dot(ones_units, p, NT, lax.Precision.HIGHEST)

        loop(per, gate_sum)
        for copy in exchange(g):
            copy.start()

        @pl.when(i > 0)
        def _():
            finish(order(i - 1 + groups))

    gp[...] = jnp.zeros_like(gp)
    loop(groups, backward)
    finish(order(groups - 1))

    acc[...] = jnp.zeros_like(acc)
    for h in range(2):
        def grads(c, h=h):
            cols = pl.ds(pl.multiple_of(c * tile, tile), tile)
            q = dot(xr[h, :, cols], gpgu[...], TN).astype(BF16)
            wg[h, cols, :] = q[:, :units]
            wu[h, cols, :] = q[:, units:]
            f = q.astype(F32)
            f = f * f
            sqs[0, h, c] = dot(ones_units, f[:, :units], NT, lax.Precision.HIGHEST)
            sqs[1, h, c] = dot(ones_units, f[:, units:], NT, lax.Precision.HIGHEST)
            d = dot(wt[...], dyr[h, :, cols], TN).astype(BF16)
            wd[:, pl.ds(pl.multiple_of(h * share + c * tile, tile), tile)] = d
            d = d.astype(F32)
            acc[...] += d * d

        loop(share // tile, grads)

    stores = [
        pltpu.make_async_copy(a, b, o_sem.at[i])
        for i, (a, b) in enumerate(((wg, ggw), (wu, guw), (wd, gdw)))
    ]
    for store in stores:
        store.start()
    squares = remote(sqs, sqr, e_sem.at[0], e_sem.at[1], tp=other)
    squares.start()
    sqd_out[...] = dot(jnp.ones((8, tile), F32), acc[...], NT, lax.Precision.HIGHEST)
    squares.wait()
    for which in range(2):
        for h in range(2):
            for c in range(share // tile):
                start = h * share + c * tile
                both = sqs[which, h, c] + sqr[which, h, c]
                sq_out[which : which + 1, start : start + tile] = both[0:1, :]
    for store in stores:
        store.wait()

    def drain(k):
        d = peer(k)
        for which, (src, dst) in enumerate(ins):
            remote(src.at[d], dst.at[t, rows(me)], s_sem.at[which, d],
                   r_sem.at[which, me], ep=d).wait_send()
        remote(sg.at[d], gr.at[me], gs_sem.at[d], gr_sem.at[me], ep=d).wait_send()
        for copy in back_copies(d):
            copy.wait_send()

    loop(n - 1, drain)

    def drain_pair(s):
        for which, (src, dst) in enumerate(ins):
            remote(dst.at[t, rows(s)], dst.at[t, rows(s)], fs_sem.at[which, s],
                   fr_sem.at[which, s], tp=other).wait_send()
        pltpu.make_async_copy(rg.at[rows(s)], back.at[s], br_sem.at[s]).wait()
        pltpu.make_async_copy(gt.at[s], gback.at[s], hr_sem.at[s]).wait()

    loop(n, drain_pair)

    def drain_group(g):
        for copy in exchange(g):
            copy.wait_send()

    loop(groups, drain_group)


def fused(n, cap, send_x, send_dy, send_gate, w_gate, w_up, w_down):
    width, units = w_gate.shape
    share = send_x.shape[2]
    total = n * cap
    groups = 8
    tile = 512
    any_spec = pl.BlockSpec(memory_space=pl.ANY)
    vmem = pl.BlockSpec(memory_space=pltpu.VMEM)
    sq_shape = (2, 2, share // tile, 8, tile)
    dma = pltpu.SemaphoreType.DMA
    shape = jax.ShapeDtypeStruct
    return pl.pallas_call(
        functools.partial(kernel, n, cap, units, share, groups, tile),
        out_shape=(
            shape((n, cap, share), BF16),
            shape((n, 8, 128), F32),
            shape((2, share, units), BF16),
            shape((2, share, units), BF16),
            shape((units, width), BF16),
            shape((2, width), F32),
            shape((8, units), F32),
        ),
        in_specs=[any_spec] * 6,
        out_specs=(any_spec,) * 5 + (vmem, vmem),
        scratch_shapes=[
            pltpu.VMEM((2, total, share), BF16),
            pltpu.VMEM((2, total, share), BF16),
            pltpu.VMEM((n, 8, 128), F32),
            pltpu.VMEM((2, share, units), BF16),
            pltpu.VMEM((2, share, units), BF16),
            pltpu.VMEM((units, width), BF16),
            pltpu.VMEM((total, units), F32),
            pltpu.VMEM((total, units), F32),
            pltpu.VMEM((total // groups, units), F32),
            pltpu.VMEM((total, 2 * units), BF16),
            pltpu.VMEM((total, units), BF16),
            pltpu.VMEM((total, share), BF16),
            pltpu.VMEM((total, share), BF16),
            pltpu.VMEM((total, share), BF16),
            pltpu.VMEM((total, share), BF16),
            pltpu.VMEM((n, 8, 128), F32),
            pltpu.VMEM((n, 8, 128), F32),
            pltpu.VMEM((n, 8, 128), F32),
            pltpu.VMEM((total, 128), F32),
            pltpu.VMEM(sq_shape, F32),
            pltpu.VMEM(sq_shape, F32),
            pltpu.VMEM((units, tile), F32),
            dma((3,)), dma((2, n)), dma((2, n)), dma((n,)), dma((n,)), dma((2, n)), dma((2, n)),
            dma((groups,)), dma((groups,)), dma((groups,)), dma((groups,)),
            dma((n,)), dma((n,)), dma((n,)), dma((n,)), dma((3,)), dma((2,)),
        ],
        compiler_params=pltpu.CompilerParams(
            collective_id=0, has_side_effects=True, vmem_limit_bytes=63 << 20
        ),
    )(send_x, send_dy, send_gate,
      w_gate.reshape(2, share, units), w_up.reshape(2, share, units), w_down)


def body(tokens, cotangent, gates, experts, gate_w, up_w, down_w):
    tok_rows, width = tokens.shape
    top_count = experts.shape[1]
    n_ep = lax.axis_size("ep")
    n_cores = lax.axis_size("tp")
    capacity = 3 * tok_rows * top_count // (2 * n_ep)
    cap = -(-capacity // 16) * 16
    n_slots = n_ep * cap
    flat_ids = experts.reshape(-1)
    onehot = (flat_ids[:, None] == jnp.arange(n_ep, dtype=jnp.int32)[None, :]).astype(jnp.int32)
    earlier = jnp.cumsum(onehot, axis=0) - onehot
    slot_of = jnp.sum(earlier * onehot, axis=1)
    target = flat_ids * cap + slot_of
    placing = (target[None, :] == jnp.arange(n_slots, dtype=jnp.int32)[:, None]).astype(F32)
    place_tok = jnp.sum(placing.reshape(n_slots, tok_rows, top_count), axis=2).astype(BF16)
    send_gate = jnp.dot(placing, gates.reshape(-1), precision=lax.Precision.HIGHEST)
    send_gate = jnp.pad(send_gate.reshape(n_ep, 1, cap), ((0, 0), (0, 7), (0, 128 - cap)))
    share = width // n_cores
    offset = lax.axis_index("tp") * share
    tok_share = lax.dynamic_slice_in_dim(tokens, offset, share, 1)
    cot_share = lax.dynamic_slice_in_dim(cotangent, offset, share, 1)
    send_x = jnp.dot(place_tok, tok_share, preferred_element_type=F32).astype(BF16)
    send_dy = jnp.dot(place_tok, cot_share, preferred_element_type=F32).astype(BF16)
    back, gback, ggw, guw, gdw, sq, sqd = fused(
        n_ep, cap, send_x.reshape(n_ep, cap, share), send_dy.reshape(n_ep, cap, share),
        send_gate, gate_w[0], up_w[0], down_w[0],
    )
    grad_tokens = lax.dot_general(
        place_tok, back.reshape(n_slots, share), TN, preferred_element_type=F32
    ).astype(BF16)
    grad_gates = jnp.dot(
        gback[:, 0, :cap].reshape(n_slots), placing, precision=lax.Precision.HIGHEST
    ).reshape(tok_rows, top_count)
    full_units = gate_w.shape[2] * n_cores
    sq = sq / full_units
    return (
        grad_tokens,
        grad_gates,
        ggw.reshape(gate_w.shape),
        guw.reshape(up_w.shape),
        gdw[None],
        sq[0][None],
        sq[1][None],
        sqd[0:1] / width,
    )


def solution(mesh):
    placed = (
        P("ep", None),
        P("ep", None),
        P("ep", None),
        P("ep", None),
        P("ep", None, "tp"),
        P("ep", None, "tp"),
        P("ep", "tp", None),
    )
    return jax.shard_map(
        body,
        mesh=mesh,
        in_specs=placed,
        out_specs=(
            P("ep", "tp"),
            P("ep", None),
            P("ep", None, "tp"),
            P("ep", None, "tp"),
            P("ep", "tp", None),
            P("ep", None),
            P("ep", None),
            P("ep", "tp"),
        ),
        check_vma=False,
    )
```
